32 devices in a mesh: ep: 8 (over z, y), tp: 4 (over x, core).
Axes of the slice: x: 2, y: 2, z: 4, core: 2. Of those that a mesh axis runs over, the one named last changes fastest.
Arguments:
- cell_query_rows: bfloat16 [2048, 2048], P('ep', 'tp'), may hold values from -6 to 6
- cell_key_rows: bfloat16 [2048, 2048], P('ep', 'tp'), may hold values from -6 to 6
- cell_value_rows: bfloat16 [2048, 2048], P('ep', 'tp'), may hold values from -6 to 6
- output_gate_logits: bfloat16 [2048, 2048], P('ep', 'tp'), may hold values from -8 to 8
- log_input_gate: float32 [8, 2048], P('tp', 'ep'), may hold values from -4 to 110
- forget_gate_logits: float32 [8, 2048], P('tp', 'ep'), may hold values from -1 to 25
- extra_log_forget: float32 [8, 2048], P('tp', 'ep'), may hold values from -0.7 to 0
- cell_output_scale: float32 [2048], P('tp'), may hold values from 0.1 to 1.9
- tokens_into_experts: bfloat16 [4096, 2048], P(('ep', 'tp')), may hold values from -6 to 6
- expert_norm_scale: float32 [2048], replicated, may hold values from 0.1 to 1.9
- token_expert_index: int32 [4096, 2], P(('ep', 'tp')), may hold values from 0 to 7, all different within a row; in each aligned block of 128 rows (0 to 127, 128 to 255, ...) at most 40 rows name the same one
- chosen_expert_weight: float32 [4096, 2], P(('ep', 'tp')), may hold values from 0.3 to 3
- expert_gate_weight: bfloat16 [8, 2048, 3584], P('ep', None, 'tp'), may hold values from -0.125 to 0.125
- expert_up_weight: bfloat16 [8, 2048, 3584], P('ep', None, 'tp'), may hold values from -0.125 to 0.125
- expert_down_weight: bfloat16 [8, 3584, 2048], P('ep', 'tp'), may hold values from -0.09375 to 0.09375
Outputs:
- gated_head_output: bfloat16 [2048, 2048], P('ep', 'tp')
- expert_output: bfloat16 [4096, 2048], P(('ep', 'tp'))
The draws below stay inside these ranges and needn't reach their ends.
Inputs may be any that keep to these rules, and one draw needn't show every extreme that they name: `token_expert_index`: each row names 2 different experts. Among the rows of one device (aligned blocks of 128 rows) no expert is named by more than 40 rows, and in every draw some expert is named by exactly 40 rows of some device.
All inputs are finite; a program needn't handle non-finite values.
Results may differ from the reference program's by a relative error of at most 0.012.
Values may be sent and summed in bfloat16 or wider, within the bound.
A program may use at most 128 MiB of HBM per device.

```python
import math
import jax
import jax.numpy as jnp
import numpy as np
from jax import lax

D = 2048
HEAD_DIM = 256
HEADS = 8
BLOCK = 64
FF = 3584
TOPK = 2
MIX_DEV = 256
MOE_DEV = 128
INNER = 2048
SEQ = 2048
EXPERTS = 8
MOE_TOK = 4096
CAP = 40
N_TP = 4


def draw_log_input_gate(key, part):
    key_base = jax.random.fold_in(jax.random.fold_in(key, 3), 0)
    return jnp.clip(jax.random.normal(key_base, (HEADS, SEQ), jnp.float32), -4.0, 4.0)


def draw_forget_gate_logits(key, part):
    subkeys = jax.random.split(jax.random.fold_in(key, 5), 4)
    slow_share = 0.5
    slow_heads = jax.random.uniform(subkeys[0], (HEADS,), jnp.float32) < slow_share
    fast_rate = jnp.exp(jax.random.uniform(subkeys[1], (HEADS,), jnp.float32, math.log(1.0 / 100.0), math.log(1.0 / 30.0)))
    head_rate = jnp.where(slow_heads, 0.5 / SEQ, fast_rate)
    segments = SEQ // MIX_DEV
    factor = jnp.exp(jax.random.uniform(subkeys[2], (segments,), jnp.float32, math.log(0.5), math.log(2.0)))
    factor = jnp.repeat(factor, MIX_DEV, total_repeat_length=SEQ)
    noise = 0.7 * jnp.clip(jax.random.normal(subkeys[3], (HEADS, SEQ), jnp.float32), -3.0, 3.0)
    return -jnp.log(head_rate[:, None] * factor[None, :]) + noise


def draw_extra_log_forget(key, part):
    key_spot, key_level = jax.random.split(jax.random.fold_in(key, 7), 2)
    spots = jax.random.randint(key_spot, (HEADS, 2), 0, SEQ)
    levels = jnp.log(jax.random.uniform(key_level, (HEADS, 2), jnp.float32, 0.5, 0.8))
    spot_hit = spots[:, :, None] == jnp.arange(SEQ)[None, None, :]
    return jnp.sum(jnp.where(spot_hit, levels[:, :, None], 0.0), axis=1)


def block_scale(own_key, extent, shards, low, top_value):
    factor_of = 1.0
    for axis_at, blocks in shards:
        heights = jax.random.uniform(jax.random.fold_in(jax.random.fold_in(own_key, 6), axis_at), (blocks,), jnp.float32, low / len(shards), top_value / len(shards))
        factor_of = factor_of * jnp.repeat(jnp.exp(heights), extent[axis_at] // blocks).reshape((-1,) + (1,) * (len(extent) - 1 - axis_at))
    return factor_of


def deal_out(rng, own, number, rows, number_of, top, limit, lean):
    sequence = jax.random.permutation(rng, number_of)
    packed, ordinary = load_shares(number_of, rows * top, limit, lean, True), load_shares(number_of, rows * top, limit, lean, False)
    places = jnp.arange(number_of)

    def named(sizes, offset_by):
        used = int((sizes > 0).sum())
        fixed = max(1, used // 4)
        moved = fixed + (places - fixed + offset_by * (used - fixed)) % max(1, number_of - fixed)
        return jnp.zeros((number_of,), jnp.int32).at[sequence[jnp.where(places < fixed, places, moved)]].set(jnp.asarray(sizes, jnp.int32))

    sizes = jnp.where(number % 4 == 0, named(packed, number // 4), named(ordinary, number - number // 4 - 1))
    mixed = jax.random.permutation(jax.random.fold_in(own, 3), number_of)
    source_of, taker = mixed[0:number_of // 2 * 2:2], mixed[1:number_of // 2 * 2:2]
    margin = jnp.minimum(sizes[source_of] - 1, limit - sizes[taker]) // 2
    margin = jnp.where((source_of == sequence[0]) | (taker == sequence[0]) | (sizes[taker] == 0), 0, jnp.maximum(margin, 0))
    moved = jax.random.randint(jax.random.fold_in(own, 4), (number_of // 2,), 0, 1 << 20) % (margin + 1)
    sizes = sizes.at[source_of].add(-moved).at[taker].add(moved)
    items = jnp.searchsorted(jnp.cumsum(sizes), jnp.arange(rows * top), side="right").astype(jnp.int32)
    listing = items.reshape(top, rows).T
    listing = listing[jax.random.permutation(jax.random.fold_in(own, 1), rows)]
    offset_by = jax.random.randint(jax.random.fold_in(own, 2), (rows, 1), 0, top)
    return jnp.take_along_axis(listing, (jnp.arange(top)[None, :] + offset_by) % top, axis=1)


def load_shares(amount, total, bound, skew, full):
    weights = [(1 << 20) // math.isqrt(grade ** skew) + 1 for grade in range(1, amount + 1)]
    largest = bound if full else min(bound, max(-(-total // amount), total * weights[0] // sum(weights)))
    least = 1 if total - largest >= amount - 1 else 0
    counts, surplus = [largest] + [least] * (amount - 1), total - largest - least * (amount - 1)
    while surplus > 0:
        candidates = [i for i in range(1, amount) if counts[i] < largest] or [i for i in range(1, amount) if counts[i] < bound]
        mass, budget = sum([weights[i] for i in candidates]), surplus
        for i in candidates:
            more = min(bound - counts[i], max(1, budget * weights[i] // mass), surplus)
            counts[i] = counts[i] + more
            surplus = surplus - more
    return np.array(counts)


def gaussian(stream_key, dims, scale, reach, cuts=(), kind=jnp.bfloat16):
    gain = block_scale(stream_key, dims, cuts, -0.22, 0.18) if cuts else 1.0
    drawn = jax.random.normal(stream_key, dims, jnp.float32) * scale * gain
    return jnp.minimum(jnp.maximum(drawn, -reach), reach).astype(kind)


def setup_inputs(seed: int = 0) -> dict:
    key_list = jax.random.split(jax.random.key(seed), 16)
    cell_query_rows = gaussian(key_list[0], (SEQ, INNER), 1.0, 6.0, ((0, 8), (1, 4)))
    cell_key_rows = gaussian(key_list[1], (SEQ, INNER), 1.0, 6.0, ((0, 8), (1, 4)))
    cell_value_rows = gaussian(key_list[2], (SEQ, INNER), 1.0, 6.0, ((0, 8), (1, 4)))
    output_gate_logits = gaussian(key_list[3], (SEQ, INNER), 1.5, 8.0, ((0, 8), (1, 4)))
    log_input_gate = draw_log_input_gate(jax.random.fold_in(key_list[15], 71), 0)
    forget_gate_logits = draw_forget_gate_logits(jax.random.fold_in(key_list[15], 71), 0)
    extra_log_forget = draw_extra_log_forget(jax.random.fold_in(key_list[15], 71), 0)
    cell_output_scale = jnp.clip(1.0 + 0.18 * jax.random.normal(key_list[7], (INNER,), jnp.float32), 0.1, 1.9)
    tokens_into_experts = gaussian(key_list[8], (MOE_TOK, D), 1.0, 6.0, ((0, 32),))
    expert_norm_scale = jnp.clip(1.0 + 0.18 * jax.random.normal(key_list[9], (D,), jnp.float32), 0.1, 1.9)
    token_expert_index_keys = jax.random.split(jax.random.fold_in(key_list[10], 1), MOE_TOK // MOE_DEV)
    token_expert_index_turns = jax.random.permutation(jax.random.fold_in(key_list[10], 3), MOE_TOK // MOE_DEV)
    token_expert_index = jax.vmap(lambda own, number: deal_out(jax.random.fold_in(key_list[10], 2), own, number, MOE_DEV, EXPERTS, TOPK, CAP, 2))(token_expert_index_keys, token_expert_index_turns).reshape((MOE_TOK, TOPK))
    chosen_expert_weight = jnp.clip(jnp.exp(math.log(3.0) - 2.3025851 * jax.random.uniform(key_list[11], (MOE_TOK, TOPK), jnp.float32) ** block_scale(key_list[11], (MOE_TOK, TOPK), ((0, 32),), -0.2, 0.2)), 0.3, 3.0)
    expert_gate_weight = gaussian(key_list[12], (EXPERTS, D, FF), D ** -0.5, 0.125, ((0, 8), (2, 4)))
    expert_up_weight = gaussian(key_list[13], (EXPERTS, D, FF), D ** -0.5, 0.125, ((0, 8), (2, 4)))
    expert_down_weight = gaussian(key_list[14], (EXPERTS, FF, D), FF ** -0.5, 0.09375, ((0, 8), (1, 4)))
    return dict(cell_query_rows=cell_query_rows, cell_key_rows=cell_key_rows, cell_value_rows=cell_value_rows, output_gate_logits=output_gate_logits, log_input_gate=log_input_gate, forget_gate_logits=forget_gate_logits, extra_log_forget=extra_log_forget, cell_output_scale=cell_output_scale, tokens_into_experts=tokens_into_experts, expert_norm_scale=expert_norm_scale, token_expert_index=token_expert_index, chosen_expert_weight=chosen_expert_weight, expert_gate_weight=expert_gate_weight, expert_up_weight=expert_up_weight, expert_down_weight=expert_down_weight)


EPSILON = 1e-06
PRECISE = lax.Precision.HIGHEST

def mixer_block(running, inputs):
    cell_state, norm_state, stabilizer = running
    queries, key_block, value_block, gate_input, forget_gate_value = inputs
    length = queries.shape[1]
    causal = jnp.tril(jnp.ones((length, length), dtype=bool))
    cumulative = jnp.cumsum(forget_gate_value, axis=-1)
    spread = jnp.where(causal, cumulative[:, :, None] - cumulative[:, None, :] + gate_input[:, None, :], -jnp.inf)
    inter_log = cumulative + stabilizer[:, None]
    row_top = jnp.maximum(inter_log, lax.optimization_barrier(jnp.max(spread, axis=-1)))
    intra_weight = jnp.exp(spread - row_top[:, :, None])
    inter_weight = jnp.exp(inter_log - row_top)
    scores = jnp.einsum('htd,hsd->hts', queries, key_block, precision=PRECISE) * intra_weight
    weights = lax.optimization_barrier(scores.astype(jnp.bfloat16)).astype(jnp.float32)
    numerator = jnp.einsum('hts,hsd->htd', weights, value_block, precision=PRECISE)
    numerator = numerator + inter_weight[:, :, None] * jnp.einsum('hvk,htk->htv', cell_state, queries, precision=PRECISE)
    denominator = lax.optimization_barrier(jnp.sum(scores, axis=-1)) + inter_weight * jnp.einsum('hk,htk->ht', norm_state, queries, precision=PRECISE)
    cell_out = numerator / jnp.maximum(jnp.abs(denominator), 1.0)[:, :, None]
    block_last = cumulative[:, -1]
    growth = block_last[:, None] - cumulative + gate_input
    new_top = jnp.maximum(block_last + stabilizer, lax.optimization_barrier(jnp.max(growth, axis=-1)))
    keep_factor = jnp.exp(block_last + stabilizer - new_top)
    shares = jnp.exp(growth - new_top[:, None])
    cell_state = keep_factor[:, None, None] * cell_state + jnp.einsum('hsv,hsk->hvk', value_block * shares[:, :, None], key_block, precision=PRECISE)
    norm_state = keep_factor[:, None] * norm_state + jnp.einsum('hs,hsk->hk', shares, key_block, precision=PRECISE)
    return ((cell_state, norm_state, new_top), cell_out)

def recurrent_cell_output(cell_query_rows, cell_key_rows, cell_value_rows, output_gate_logits, log_input_gate, forget_gate_logits, extra_log_forget, cell_output_scale):
    seq_len, row_width = cell_query_rows.shape
    head_count = row_width // HEAD_DIM
    block_count = seq_len // BLOCK

    def to_blocks(array):
        return array.astype(jnp.float32).reshape(block_count, BLOCK, head_count, HEAD_DIM).transpose(0, 2, 1, 3)

    def gate_blocks(array):
        return array.reshape(head_count, block_count, BLOCK).transpose(1, 0, 2)
    forget_log_value = jax.nn.log_sigmoid(forget_gate_logits) + extra_log_forget
    start_state = (jnp.zeros((head_count, HEAD_DIM, HEAD_DIM), jnp.float32), jnp.zeros((head_count, HEAD_DIM), jnp.float32), jnp.zeros((head_count,), jnp.float32))
    inputs = (to_blocks(cell_query_rows), to_blocks(cell_key_rows) * HEAD_DIM ** (-0.5), to_blocks(cell_value_rows), gate_blocks(log_input_gate), gate_blocks(forget_log_value))
    _, outputs = lax.scan(mixer_block, start_state, inputs)
    cell_out = outputs.transpose(0, 2, 1, 3).reshape(seq_len, row_width)
    gated = cell_out * cell_output_scale * jax.nn.sigmoid(output_gate_logits.astype(jnp.float32))
    return gated.astype(jnp.bfloat16)

def slot_tables(ids, experts, capacity):
    flat_ids = ids.reshape(-1)
    onehot = (flat_ids[:, None] == jnp.arange(experts, dtype=jnp.int32)[None, :]).astype(jnp.int32)
    earlier = jnp.cumsum(onehot, axis=0) - onehot
    rank_in = lax.optimization_barrier(jnp.sum(earlier * onehot, axis=1))
    slot_index = flat_ids * capacity + rank_in
    token_of = jnp.arange(flat_ids.shape[0], dtype=jnp.int32) // ids.shape[1]
    slot_hit = slot_index[:, None] == jnp.arange(experts * capacity, dtype=jnp.int32)[None, :]
    slot_owner = lax.optimization_barrier(jnp.sum(jnp.where(slot_hit, token_of[:, None] + 1, 0), axis=0)).astype(jnp.int32)
    return (slot_owner, slot_index.reshape(ids.shape).astype(jnp.int32))

def experts_part(tokens_into_experts, expert_norm_scale, token_expert_index, chosen_expert_weight, expert_gate_weight, expert_up_weight, expert_down_weight):
    input_float = tokens_into_experts.astype(jnp.float32)
    normed = (input_float * lax.rsqrt(lax.optimization_barrier(jnp.mean(input_float * input_float, axis=-1, keepdims=True)) + EPSILON) * expert_norm_scale).astype(jnp.bfloat16)
    block_total = MOE_TOK // MOE_DEV
    block_ids = token_expert_index.reshape(block_total, MOE_DEV, TOPK)

    def tables(ids):
        return slot_tables(ids, EXPERTS, CAP)
    slot_owner, slot_index = jax.vmap(tables)(block_ids)
    offsets = jnp.arange(block_total, dtype=jnp.int32) * MOE_DEV
    owner_view = slot_owner.reshape(block_total, EXPERTS, CAP).transpose(1, 0, 2)
    row_index = jnp.where(owner_view > 0, owner_view - 1 + offsets[None, :, None], -1).reshape(EXPERTS, block_total * CAP)
    quarter = FF // N_TP

    def one_expert(inputs):
        index_rows, gate_matrix, up_matrix, down_matrix = inputs
        routed_rows = jnp.where((index_rows >= 0)[:, None], normed[jnp.maximum(index_rows, 0)], jnp.zeros((), jnp.bfloat16))
        gate_out = jnp.dot(routed_rows, gate_matrix, preferred_element_type=jnp.float32)
        up_out = jnp.dot(routed_rows, up_matrix, preferred_element_type=jnp.float32)
        hidden = (jax.nn.silu(gate_out) * up_out).astype(jnp.bfloat16)
        summed = jnp.zeros((routed_rows.shape[0], down_matrix.shape[1]), jnp.float32)
        for group_index in range(N_TP):
            term = jnp.dot(hidden[:, group_index * quarter:(group_index + 1) * quarter], down_matrix[group_index * quarter:(group_index + 1) * quarter], preferred_element_type=jnp.float32).astype(jnp.bfloat16)
            summed = summed + lax.optimization_barrier(term).astype(jnp.float32)
        return summed.astype(jnp.bfloat16)
    results = lax.map(one_expert, (row_index, expert_gate_weight, expert_up_weight, expert_down_weight))
    rank_in = slot_index - block_ids * CAP
    position = jnp.arange(block_total, dtype=jnp.int32)[:, None, None] * CAP + rank_in
    picked = results[block_ids, position]
    weights = chosen_expert_weight.reshape(block_total, MOE_DEV, TOPK)
    combined = lax.optimization_barrier(jnp.sum(weights[..., None] * picked.astype(jnp.float32), axis=2))
    return combined.reshape(MOE_TOK, picked.shape[-1]).astype(jnp.bfloat16)

def reference(cell_query_rows, cell_key_rows, cell_value_rows, output_gate_logits, log_input_gate, forget_gate_logits, extra_log_forget, cell_output_scale, tokens_into_experts, expert_norm_scale, token_expert_index, chosen_expert_weight, expert_gate_weight, expert_up_weight, expert_down_weight):
    gated_head_output = recurrent_cell_output(cell_query_rows, cell_key_rows, cell_value_rows, output_gate_logits, log_input_gate, forget_gate_logits, extra_log_forget, cell_output_scale)
    expert_output = experts_part(tokens_into_experts, expert_norm_scale, token_expert_index, chosen_expert_weight, expert_gate_weight, expert_up_weight, expert_down_weight)
    return (gated_head_output, expert_output)
```

```python
import functools

import jax
import jax.numpy as jnp
from jax import lax
from jax.experimental import pallas as pl
from jax.experimental.pallas import tpu as pltpu
from jax.sharding import PartitionSpec as P

HEAD_DIM = 256
BLOCK = 64
TOPK = 2


EPSILON = 1e-06
PRECISE = lax.Precision.HIGHEST


def carried_in(x, axis, combine, identity):
    size, here = (lax.axis_size(axis), lax.axis_index(axis))
    everything = jax.tree.map(lambda part: lax.all_gather(part, axis), x)
    start = identity

    def step(k, before):
        reached = k < here
        new = combine(before, jax.tree.map(lambda part: part[k], everything))
        return jax.tree.map(lambda a, b: jnp.where(reached, a, b), new, before)

    return lax.fori_loop(0, size, step, start)


def combine(earlier, later):
    cell_early, norm_early, stab_early, total_early = earlier
    cell_late, norm_late, stab_late, total_late = later
    stabilizer = jnp.maximum(total_late + stab_early, stab_late)
    keep_factor = jnp.exp(total_late + stab_early - stabilizer)
    take_factor = jnp.exp(stab_late - stabilizer)
    cell_state = (
        keep_factor[..., None, None] * cell_early + take_factor[..., None, None] * cell_late
    )
    norm_state = keep_factor[..., None] * norm_early + take_factor[..., None] * norm_late
    return (cell_state, norm_state, stabilizer, total_early + total_late)


def mix_heads(
    cell_query_rows,
    cell_key_rows,
    cell_value_rows,
    output_gate_logits,
    log_input_gate,
    forget_gate_logits,
    extra_log_forget,
    cell_output_scale,
):
    n_tok, row_width = cell_query_rows.shape
    head_count = row_width // HEAD_DIM
    block_count = n_tok // BLOCK
    key_scale = HEAD_DIM ** (-0.5)
    block_shape = (block_count, BLOCK, head_count, HEAD_DIM)
    query_blocks = cell_query_rows.reshape(block_shape)
    key_blocks = cell_key_rows.reshape(block_shape)
    value_blocks = cell_value_rows.reshape(block_shape)
    gate_input = log_input_gate.reshape(head_count, block_count, BLOCK)
    forget_gate_value = (jax.nn.log_sigmoid(forget_gate_logits) + extra_log_forget).reshape(
        head_count, block_count, BLOCK
    )
    cumulative = jnp.cumsum(forget_gate_value, axis=-1)
    block_last = cumulative[..., -1]
    growth = block_last[..., None] - cumulative + gate_input
    block_top = jnp.max(growth, axis=-1)
    shares = jnp.exp(growth - block_top[..., None])
    key_float = key_blocks.astype(jnp.float32) * key_scale
    value_weighted = value_blocks.astype(jnp.float32) * shares.transpose(1, 2, 0)[..., None]
    cell_terms = jnp.einsum("bshv,bshk->bhvk", value_weighted, key_float, precision=PRECISE)
    norm_terms = jnp.einsum("hbs,bshk->bhk", shares, key_float, precision=PRECISE)
    block_terms = (cell_terms, norm_terms, block_top.T, block_last.T)
    identity_state = (
        jnp.zeros((head_count, HEAD_DIM, HEAD_DIM), jnp.float32),
        jnp.zeros((head_count, HEAD_DIM), jnp.float32),
        jnp.full((head_count,), -1e30, jnp.float32),
        jnp.zeros((head_count,), jnp.float32),
    )

    def fold_step(running, block_term):
        return (combine(running, block_term), running)

    device_total, before = lax.scan(fold_step, identity_state, block_terms)
    sent_state = (device_total[0].astype(jnp.bfloat16),) + device_total[1:]
    prior_state = carried_in(sent_state, "ep", combine, identity_state)
    zero_state = (
        jnp.zeros((head_count, HEAD_DIM, HEAD_DIM), jnp.float32),
        jnp.zeros((head_count, HEAD_DIM), jnp.float32),
        jnp.zeros((head_count,), jnp.float32),
        jnp.zeros((head_count,), jnp.float32),
    )
    start_state = combine(zero_state, prior_state)
    cell_state, norm_state, stabilizer, _ = combine(start_state, before)
    inter_log = cumulative + stabilizer.T[:, :, None]
    causal = jnp.tril(jnp.ones((BLOCK, BLOCK), dtype=bool))
    spread = jnp.where(
        causal,
        cumulative[..., :, None] - cumulative[..., None, :] + gate_input[..., None, :],
        -jnp.inf,
    )
    row_top = jnp.maximum(inter_log, jnp.max(spread, axis=-1))
    intra_weight = jnp.exp(spread - row_top[..., None])
    inter_weight = jnp.exp(inter_log - row_top)
    scores = (
        jnp.einsum("bthd,bshd->hbts", query_blocks, key_blocks, preferred_element_type=jnp.float32)
        * key_scale
        * intra_weight
    )
    weights = scores.astype(jnp.bfloat16)
    numerator = jnp.einsum(
        "hbts,bshd->hbtd", weights, value_blocks, preferred_element_type=jnp.float32
    )
    query_float = query_blocks.astype(jnp.float32)
    numerator = numerator + inter_weight[..., None] * jnp.einsum(
        "bhvk,bthk->hbtv", cell_state, query_float, precision=PRECISE
    )
    denominator = jnp.sum(scores, axis=-1) + inter_weight * jnp.einsum(
        "bhk,bthk->hbt", norm_state, query_float, precision=PRECISE
    )
    cell_out = numerator / jnp.maximum(jnp.abs(denominator), 1.0)[..., None]
    cell_out = cell_out.transpose(1, 2, 0, 3).reshape(n_tok, row_width)
    return (
        cell_out * cell_output_scale * jax.nn.sigmoid(output_gate_logits.astype(jnp.float32))
    ).astype(jnp.bfloat16)


def slot_tables(ids, experts, capacity):
    flat_ids = ids.reshape(-1)
    onehot = (flat_ids[:, None] == jnp.arange(experts, dtype=jnp.int32)[None, :]).astype(jnp.int32)
    earlier = jnp.cumsum(onehot, axis=0) - onehot
    rank_in = jnp.sum(earlier * onehot, axis=1)
    slot_index = flat_ids * capacity + rank_in
    token_of = jnp.arange(flat_ids.shape[0], dtype=jnp.int32) // ids.shape[1]
    slot_hit = slot_index[:, None] == jnp.arange(experts * capacity, dtype=jnp.int32)[None, :]
    slot_owner = jnp.sum(jnp.where(slot_hit, token_of[:, None] + 1, 0), axis=0)
    return (slot_owner, slot_index.reshape(ids.shape))


MESH = pl.DeviceIdType.MESH
LANES = 128


def expert_kernel(
    n_ep,
    send_ref,
    gate_hbm,
    up_hbm,
    down_hbm,
    ret_ref,
    disp,
    part,
    first,
    pair_sum,
    second,
    final,
    rows_in,
    hidden,
    gate_up,
    down,
    weight_sem,
    local_sem,
    sem_a_send,
    sem_a_recv,
    sem_x_send,
    sem_x_recv,
    sem_c_send,
    sem_c_recv,
    sem_d_send,
    sem_d_recv,
    sem_f_send,
    sem_f_recv,
    sem_s_send,
    sem_s_recv,
    sem_r_send,
    sem_r_recv,
):
    e, t = lax.axis_index("ep"), lax.axis_index("tp")
    partner = t + 1 - 2 * (t % 2)
    across = (t + 2) % 4
    cap, width = send_ref.shape[1], send_ref.shape[2]
    tiles, outs = gate_up.shape[0], down.shape[0]
    out_cols = down.shape[2]

    def remote(src, dst, ssem, rsem, dev):
        return pltpu.make_async_remote_copy(
            src_ref=src, dst_ref=dst, send_sem=ssem, recv_sem=rsem, device_id=dev, device_id_type=MESH
        )

    barrier = pltpu.get_barrier_semaphore()
    for k in range(1, n_ep):
        pl.semaphore_signal(barrier, inc=1, device_id=((e + k) % n_ep, t), device_id_type=MESH)
    for other in (partner, across):
        pl.semaphore_signal(barrier, inc=1, device_id=(e, other), device_id_type=MESH)

    weights = []
    for j in range(tiles):
        cols = pl.ds(j * LANES, LANES)
        weights.append(
            pltpu.make_async_copy(gate_hbm.at[:, cols], gate_up.at[j, :, pl.ds(0, LANES)], weight_sem.at[3 * j])
        )
        weights.append(
            pltpu.make_async_copy(up_hbm.at[:, cols], gate_up.at[j, :, pl.ds(LANES, LANES)], weight_sem.at[3 * j + 1])
        )
    for j in range(outs):
        weights.append(
            pltpu.make_async_copy(
                down_hbm.at[:, pl.ds(j * out_cols, out_cols)], down.at[j], weight_sem.at[3 * tiles + j]
            )
        )
    local = pltpu.make_async_copy(send_ref.at[0], disp.at[0, 0], local_sem)
    local.start()
    pl.semaphore_wait(barrier, n_ep + 1)

    def out_copy(k):
        return remote(send_ref.at[k], disp.at[k, 0], sem_a_send.at[k], sem_a_recv.at[k], ((e + k) % n_ep, t))

    def to_across(k):
        return remote(disp.at[k, 0], disp.at[k, 1], sem_x_send.at[k], sem_x_recv.at[k], (e, across))

    def to_partner_own(k):
        return remote(disp.at[k, 0], disp.at[k, 2], sem_c_send.at[k], sem_c_recv.at[k], (e, partner))

    def to_partner_far(k):
        return remote(disp.at[k, 1], disp.at[k, 3], sem_d_send.at[k], sem_d_recv.at[k], (e, partner))

    def sum_to_partner(k):
        return remote(part.at[k, pl.ds(2, 2)], first.at[k], sem_f_send.at[k], sem_f_recv.at[k], (e, partner))

    def sum_across(k):
        return remote(pair_sum.at[k], second.at[k], sem_s_send.at[k], sem_s_recv.at[k], (e, across))

    def give_back(k):
        return remote(final.at[k], ret_ref.at[k], sem_r_send.at[k], sem_r_recv.at[k], ((e + n_ep - k) % n_ep, t))

    half = n_ep // 2
    for k in range(half):
        out_copy(k + half).start()
        if k:
            out_copy(k).start()
    for copy in weights:
        copy.start()

    def spread_own(i):
        for k in (i, i + half):
            if k:
                out_copy(k).wait_recv()
            else:
                local.wait()
            to_across(k).start()
            to_partner_own(k).start()

    def spread_far(i):
        for k in (i, i + half):
            to_across(k).wait_recv()
            to_partner_far(k).start()

    def all_here(i):
        for k in (i, i + half):
            to_partner_own(k).wait_recv()
            to_partner_far(k).wait_recv()

    def wide(block):
        return block.astype(jnp.float32)

    def sum_pairs(i):
        for k in (i, i + half):
            sum_to_partner(k).wait_recv()
            pair_sum[k] = (wide(part[k, 1]) + wide(first[k, 1])).astype(jnp.bfloat16)
            sum_across(k).start()

    def sum_rest(i):
        for k in (i, i + half):
            sum_across(k).wait_recv()
            done = (wide(part[k, 0]) + wide(first[k, 0]) + wide(second[k])).astype(jnp.bfloat16)
            if k:
                final[k] = done
                give_back(k).start()
            else:
                ret_ref[0] = done

    def hidden_units(i):
        for at, k in enumerate((i, i + half)):
            block = jnp.concatenate([wide(disp[k, j]) for j in range(4)], axis=0)
            rows_in[pl.ds(at * 4 * cap, 4 * cap)] = block.astype(jnp.bfloat16)

        def step(j, carry):
            both = jnp.dot(rows_in[...], gate_up[j], preferred_element_type=jnp.float32)
            gate_out, up_out = both[:, :LANES], both[:, LANES:]
            hidden[j] = (jax.nn.silu(gate_out) * up_out).astype(jnp.bfloat16)
            return carry

        lax.fori_loop(0, tiles, step, 0)

    def results(i):
        units = jnp.concatenate([hidden[j] for j in range(tiles)], axis=1)

        def step(j, carry):
            out = jnp.dot(units, down[j], preferred_element_type=jnp.float32)
            cols = pl.ds(pl.multiple_of(j * out_cols, out_cols), out_cols)
            for at, k in enumerate((i, i + half)):
                for m in range(4):
                    lo = (at * 4 + m) * cap
                    part[k, m, :, cols] = out[lo : lo + cap].astype(jnp.bfloat16)
            return carry

        lax.fori_loop(0, outs, step, 0)

    spread_own(0)
    spread_far(0)
    for i in range(half):
        all_here(i)
        if i == 0:
            for copy in weights:
                copy.wait()
        if i + 1 < half:
            spread_own(i + 1)
        hidden_units(i)
        if i:
            sum_pairs(i - 1)
        results(i)
        for k in (i, i + half):
            sum_to_partner(k).start()
        if i + 1 < half:
            spread_far(i + 1)
        if i:
            sum_rest(i - 1)
    sum_pairs(half - 1)
    sum_rest(half - 1)
    for k in range(n_ep):
        if k:
            give_back(k).wait_recv()
            out_copy(k).wait_send()
            give_back(k).wait_send()
        to_across(k).wait_send()
        to_partner_own(k).wait_send()
        to_partner_far(k).wait_send()
        sum_to_partner(k).wait_send()
        sum_across(k).wait_send()


def experts_by_kernel(sendbuf, gate_matrix, up_matrix, down_matrix, n_ep):
    rows, width = sendbuf.shape
    cap = rows // n_ep
    units = gate_matrix.shape[1]
    tiles, out_cols = units // LANES, 256
    block = (n_ep, cap, width)
    vmem = pltpu.VMEM
    bf16 = jnp.bfloat16
    dma = pltpu.SemaphoreType.DMA
    return pl.pallas_call(
        functools.partial(expert_kernel, n_ep),
        out_shape=jax.ShapeDtypeStruct(block, bf16),
        in_specs=[pl.BlockSpec(memory_space=pltpu.VMEM)] + [pl.BlockSpec(memory_space=pl.ANY)] * 3,
        out_specs=pl.BlockSpec(memory_space=pltpu.VMEM),
        scratch_shapes=[
            vmem((n_ep, 4, cap, width), bf16),
            vmem((n_ep, 4, cap, width), bf16),
            vmem((n_ep, 2, cap, width), bf16),
            vmem(block, bf16),
            vmem(block, bf16),
            vmem(block, bf16),
            vmem((8 * cap, width), bf16),
            vmem((tiles, 8 * cap, LANES), bf16),
            vmem((tiles, width, 2 * LANES), bf16),
            vmem((width // out_cols, units, out_cols), bf16),
            dma((3 * tiles + width // out_cols,)),
            dma,
        ]
        + [dma((n_ep,))] * 14,
        compiler_params=pltpu.CompilerParams(
            collective_id=0, has_side_effects=True, vmem_limit_bytes=56 * 1024 * 1024
        ),
        cost_estimate=pl.CostEstimate(
            flops=24 * rows * width * units, bytes_accessed=6 * width * units, transcendentals=4 * rows * units
        ),
    )(sendbuf.reshape(block), gate_matrix, up_matrix, down_matrix).reshape(rows, width)


def local(
    cell_query_rows,
    cell_key_rows,
    cell_value_rows,
    output_gate_logits,
    log_input_gate,
    forget_gate_logits,
    extra_log_forget,
    cell_output_scale,
    tokens_into_experts,
    expert_norm_scale,
    token_expert_index,
    chosen_expert_weight,
    expert_gate_weight,
    expert_up_weight,
    expert_down_weight,
):
    gated_head_output = mix_heads(
        cell_query_rows,
        cell_key_rows,
        cell_value_rows,
        output_gate_logits,
        log_input_gate,
        forget_gate_logits,
        extra_log_forget,
        cell_output_scale,
    )
    ep_count = lax.axis_size("ep")
    n_tok = tokens_into_experts.shape[0]
    experts = ep_count * expert_gate_weight.shape[0]
    capacity = n_tok * TOPK * 5 // (4 * experts)
    input_float = tokens_into_experts.astype(jnp.float32)
    normed = (
        input_float
        * lax.rsqrt(jnp.mean(input_float * input_float, axis=-1, keepdims=True) + EPSILON)
        * expert_norm_scale
    ).astype(jnp.bfloat16)
    gate_matrix = expert_gate_weight[0]
    up_matrix = expert_up_weight[0]
    down_matrix = expert_down_weight[0]
    by_kernel = (
        lax.axis_size("tp") == 4
        and ep_count % 2 == 0
        and capacity % 8 == 0
        and gate_matrix.shape[1] % LANES == 0
        and gate_matrix.shape[0] % 256 == 0
    )
    if by_kernel:
        token_expert_index = (token_expert_index + ep_count - lax.axis_index("ep")) % ep_count
    slot_owner, slot_index = slot_tables(token_expert_index, experts, capacity)
    sendbuf = jnp.where(
        (slot_owner > 0)[:, None],
        normed[jnp.maximum(slot_owner - 1, 0)],
        jnp.zeros((), jnp.bfloat16),
    )
    if by_kernel:
        returned = experts_by_kernel(sendbuf, gate_matrix, up_matrix, down_matrix, ep_count)
    else:
        arrived = lax.all_to_all(sendbuf, "ep", split_axis=0, concat_axis=0, tiled=True)
        routed_rows = lax.all_gather(arrived, "tp", axis=0, tiled=True)
        gate_out = jnp.dot(routed_rows, gate_matrix, preferred_element_type=jnp.float32)
        up_out = jnp.dot(routed_rows, up_matrix, preferred_element_type=jnp.float32)
        hidden = (jax.nn.silu(gate_out) * up_out).astype(jnp.bfloat16)
        summed = lax.psum_scatter(
            jnp.dot(hidden, down_matrix, preferred_element_type=jnp.float32).astype(jnp.bfloat16),
            "tp",
            scatter_dimension=0,
            tiled=True,
        )
        returned = lax.all_to_all(summed, "ep", split_axis=0, concat_axis=0, tiled=True)
    picked = returned[slot_index]
    expert_output = jnp.sum(
        chosen_expert_weight[..., None] * picked.astype(jnp.float32), axis=1
    ).astype(jnp.bfloat16)
    return (gated_head_output, expert_output)


def solution(mesh):
    return jax.shard_map(
        local,
        mesh=mesh,
        in_specs=(
            P("ep", "tp"),
            P("ep", "tp"),
            P("ep", "tp"),
            P("ep", "tp"),
            P("tp", "ep"),
            P("tp", "ep"),
            P("tp", "ep"),
            P("tp"),
            P(("ep", "tp"), None),
            P(),
            P(("ep", "tp"), None),
            P(("ep", "tp"), None),
            P("ep", None, "tp"),
            P("ep", None, "tp"),
            P("ep", "tp", None),
        ),
        out_specs=(P("ep", "tp"), P(("ep", "tp"), None)),
        check_vma=False,
    )
```

```python
import functools

import jax
import jax.numpy as jnp
from jax import lax
from jax.experimental import pallas as pl
from jax.experimental.pallas import tpu as pltpu
from jax.sharding import PartitionSpec as P

HEAD_DIM = 256
BLOCK = 64
TOPK = 2


EPSILON = 1e-06
PRECISE = lax.Precision.HIGHEST


def carried_in(x, axis, combine, identity):
    size, here = (lax.axis_size(axis), lax.axis_index(axis))
    everything = jax.tree.map(lambda part: lax.all_gather(part, axis), x)
    start = identity

    def step(k, before):
        reached = k < here
        new = combine(before, jax.tree.map(lambda part: part[k], everything))
        return jax.tree.map(lambda a, b: jnp.where(reached, a, b), new, before)

    return lax.fori_loop(0, size, step, start)


def gathered_carry(device_total):
    cell, norm, stab, total = device_total
    zeros = tuple(jnp.zeros_like(part) for part in device_total)
    identity = zeros[:2] + (jnp.full_like(stab, -1e30),) + zeros[3:]
    sent_state = (cell.astype(jnp.bfloat16), norm, stab, total)
    return combine(zeros, carried_in(sent_state, "ep", combine, identity))


def combine(earlier, later):
    cell_early, norm_early, stab_early, total_early = earlier
    cell_late, norm_late, stab_late, total_late = later
    stabilizer = jnp.maximum(total_late + stab_early, stab_late)
    keep_factor = jnp.exp(total_late + stab_early - stabilizer)
    take_factor = jnp.exp(stab_late - stabilizer)
    cell_state = (
        keep_factor[..., None, None] * cell_early + take_factor[..., None, None] * cell_late
    )
    norm_state = keep_factor[..., None] * norm_early + take_factor[..., None] * norm_late
    return (cell_state, norm_state, stabilizer, total_early + total_late)


def mix_heads(
    cell_query_rows,
    cell_key_rows,
    cell_value_rows,
    output_gate_logits,
    log_input_gate,
    forget_gate_logits,
    extra_log_forget,
    cell_output_scale,
    carry,
):
    n_tok, row_width = cell_query_rows.shape
    head_count = row_width // HEAD_DIM
    block_count = n_tok // BLOCK
    key_scale = HEAD_DIM ** (-0.5)
    block_shape = (block_count, BLOCK, head_count, HEAD_DIM)
    query_blocks = cell_query_rows.reshape(block_shape)
    key_blocks = cell_key_rows.reshape(block_shape)
    value_blocks = cell_value_rows.reshape(block_shape)
    gate_input = log_input_gate.reshape(head_count, block_count, BLOCK)
    forget_gate_value = (jax.nn.log_sigmoid(forget_gate_logits) + extra_log_forget).reshape(
        head_count, block_count, BLOCK
    )
    cumulative = jnp.cumsum(forget_gate_value, axis=-1)
    block_last = cumulative[..., -1]
    growth = block_last[..., None] - cumulative + gate_input
    block_top = jnp.max(growth, axis=-1)
    shares = jnp.exp(growth - block_top[..., None])
    key_float = key_blocks.astype(jnp.float32) * key_scale
    value_weighted = value_blocks.astype(jnp.float32) * shares.transpose(1, 2, 0)[..., None]
    cell_terms = jnp.einsum("bshv,bshk->bhvk", value_weighted, key_float, precision=PRECISE)
    norm_terms = jnp.einsum("hbs,bshk->bhk", shares, key_float, precision=PRECISE)
    block_terms = (cell_terms, norm_terms, block_top.T, block_last.T)
    identity_state = (
        jnp.zeros((head_count, HEAD_DIM, HEAD_DIM), jnp.float32),
        jnp.zeros((head_count, HEAD_DIM), jnp.float32),
        jnp.full((head_count,), -1e30, jnp.float32),
        jnp.zeros((head_count,), jnp.float32),
    )

    def fold_step(running, block_term):
        return (combine(running, block_term), running)

    device_total, before = lax.scan(fold_step, identity_state, block_terms, unroll=True)
    start_state = carry(device_total)
    cell_state, norm_state, stabilizer, _ = combine(start_state, before)
    inter_log = cumulative + stabilizer.T[:, :, None]
    causal = jnp.tril(jnp.ones((BLOCK, BLOCK), dtype=bool))
    spread = jnp.where(
        causal,
        cumulative[..., :, None] - cumulative[..., None, :] + gate_input[..., None, :],
        -jnp.inf,
    )
    row_top = jnp.maximum(inter_log, jnp.max(spread, axis=-1))
    intra_weight = jnp.exp(spread - row_top[..., None])
    inter_weight = jnp.exp(inter_log - row_top)
    scores = (
        jnp.einsum("bthd,bshd->hbts", query_blocks, key_blocks, preferred_element_type=jnp.float32)
        * key_scale
        * intra_weight
    )
    weights = scores.astype(jnp.bfloat16)
    numerator = jnp.einsum(
        "hbts,bshd->hbtd", weights, value_blocks, preferred_element_type=jnp.float32
    )
    query_float = query_blocks.astype(jnp.float32)
    numerator = numerator + inter_weight[..., None] * jnp.einsum(
        "bhvk,bthk->hbtv", cell_state, query_float, precision=PRECISE
    )
    denominator = jnp.sum(scores, axis=-1) + inter_weight * jnp.einsum(
        "bhk,bthk->hbt", norm_state, query_float, precision=PRECISE
    )
    cell_out = numerator / jnp.maximum(jnp.abs(denominator), 1.0)[..., None]
    cell_out = cell_out.transpose(1, 2, 0, 3).reshape(n_tok, row_width)
    return (
        cell_out * cell_output_scale * jax.nn.sigmoid(output_gate_logits.astype(jnp.float32))
    ).astype(jnp.bfloat16)


def slot_masks(ids, experts, capacity):
    n_tok = ids.shape[0]
    slots = jnp.arange(experts * capacity, dtype=jnp.int32)[None, :]
    slot_expert, slot_rank = slots // capacity, slots % capacity
    chosen = [ids[:, j : j + 1] == slot_expert for j in range(ids.shape[1])]
    named = functools.reduce(jnp.logical_or, chosen)
    earlier = jnp.tril(jnp.ones((n_tok, n_tok), jnp.bfloat16), -1)
    rank = jnp.dot(earlier, named.astype(jnp.bfloat16), preferred_element_type=jnp.float32)
    hit = jnp.logical_and(named, rank == slot_rank.astype(jnp.float32))
    return hit, chosen


MESH = pl.DeviceIdType.MESH
LANES = 128


def expert_kernel(
    n_ep,
    heads,
    send_ref,
    mine_c,
    mine_aux,
    gate_hbm,
    up_hbm,
    down_hbm,
    ret_ref,
    in_c,
    in_aux,
    disp,
    part,
    first,
    pair_sum,
    second,
    final,
    rows_in,
    hidden,
    gate_up,
    down,
    other_c,
    other_aux,
    pair_c,
    pair_aux,
    next_c,
    next_aux,
    chain_c,
    chain_aux,
    state_send,
    state_recv,
    weight_sem,
    local_sem,
    sem_a_send,
    sem_a_recv,
    sem_x_send,
    sem_x_recv,
    sem_c_send,
    sem_c_recv,
    sem_d_send,
    sem_d_recv,
    sem_f_send,
    sem_f_recv,
    sem_s_send,
    sem_s_recv,
    sem_r_send,
    sem_r_recv,
):
    e, t = lax.axis_index("ep"), lax.axis_index("tp")
    partner = t + 1 - 2 * (t % 2)
    across = (t + 2) % 4
    cap, width = send_ref.shape[1], send_ref.shape[2]
    tiles, outs = gate_up.shape[0], down.shape[0]
    out_cols = down.shape[2]

    def remote(src, dst, ssem, rsem, dev):
        return pltpu.make_async_remote_copy(
            src_ref=src, dst_ref=dst, send_sem=ssem, recv_sem=rsem, device_id=dev, device_id_type=MESH
        )

    barrier = pltpu.get_barrier_semaphore()
    for k in range(1, n_ep):
        pl.semaphore_signal(barrier, inc=1, device_id=((e + k) % n_ep, t), device_id_type=MESH)
    for other in (partner, across):
        pl.semaphore_signal(barrier, inc=1, device_id=(e, other), device_id_type=MESH)

    weights = []
    for j in range(tiles):
        cols = pl.ds(j * LANES, LANES)
        weights.append(
            pltpu.make_async_copy(gate_hbm.at[:, cols], gate_up.at[j, :, pl.ds(0, LANES)], weight_sem.at[3 * j])
        )
        weights.append(
            pltpu.make_async_copy(up_hbm.at[:, cols], gate_up.at[j, :, pl.ds(LANES, LANES)], weight_sem.at[3 * j + 1])
        )
    for j in range(outs):
        weights.append(
            pltpu.make_async_copy(
                down_hbm.at[:, pl.ds(j * out_cols, out_cols)], down.at[j], weight_sem.at[3 * tiles + j]
            )
        )
    local = pltpu.make_async_copy(send_ref.at[0], disp.at[0, 0], local_sem)
    local.start()
    pl.semaphore_wait(barrier, n_ep + 1)

    def out_copy(k):
        return remote(send_ref.at[k], disp.at[k, 0], sem_a_send.at[k], sem_a_recv.at[k], ((e + k) % n_ep, t))

    def to_across(k):
        return remote(disp.at[k, 0], disp.at[k, 1], sem_x_send.at[k], sem_x_recv.at[k], (e, across))

    def to_partner_own(k):
        return remote(disp.at[k, 0], disp.at[k, 2], sem_c_send.at[k], sem_c_recv.at[k], (e, partner))

    def to_partner_far(k):
        return remote(disp.at[k, 1], disp.at[k, 3], sem_d_send.at[k], sem_d_recv.at[k], (e, partner))

    def sum_to_partner(k):
        return remote(part.at[k, pl.ds(2, 2)], first.at[k], sem_f_send.at[k], sem_f_recv.at[k], (e, partner))

    def sum_across(k):
        return remote(pair_sum.at[k], second.at[k], sem_s_send.at[k], sem_s_recv.at[k], (e, across))

    def give_back(k):
        return remote(final.at[k], ret_ref.at[k], sem_r_send.at[k], sem_r_recv.at[k], ((e + n_ep - k) % n_ep, t))

    half = n_ep // 2
    side, step_at = e % 2, e // 2
    pair_copies = [
        remote(mine_c, other_c, state_send.at[0], state_recv.at[0], (e + 1 - 2 * side, t)),
        remote(mine_aux, other_aux, state_send.at[1], state_recv.at[1], (e + 1 - 2 * side, t)),
    ]
    chain_copies = [
        remote(next_c, chain_c, state_send.at[2], state_recv.at[2], ((e + 2) % n_ep, t)),
        remote(next_aux, chain_aux, state_send.at[3], state_recv.at[3], ((e + 2) % n_ep, t)),
    ]

    def matrix(ref, h):
        size = ref.shape[0] // heads
        return ref[h * size : (h + 1) * size].astype(jnp.float32)

    def state(c_ref, aux_ref, h):
        n, m, total = (aux_ref[g * heads + h : g * heads + h + 1] for g in range(3))
        return matrix(c_ref, h), n, m, total

    def joined(early, late):
        top = jnp.maximum(late[3] + early[2], late[2])
        keep, take = jnp.exp(late[3] + early[2] - top), jnp.exp(late[2] - top)
        return keep * early[0] + take * late[0], keep * early[1] + take * late[1], top, early[3] + late[3]

    def put(c_ref, aux_ref, h, parts):
        size = c_ref.shape[0] // heads
        c_ref[h * size : (h + 1) * size] = parts[0].astype(c_ref.dtype)
        for g in range(3):
            aux_ref[g * heads + h : g * heads + h + 1] = parts[g + 1]

    def pair_total():
        for copy in pair_copies:
            copy.wait_recv()
        for h in range(heads):
            mine, other = state(mine_c, mine_aux, h), state(other_c, other_aux, h)
            early = [jnp.where(side == 0, a, b) for a, b in zip(mine, other)]
            late = [jnp.where(side == 0, b, a) for a, b in zip(mine, other)]
            put(pair_c, pair_aux, h, joined(early, late))

    def chain(i):
        @pl.when(step_at == i)
        def _():
            if i:
                for copy in chain_copies:
                    copy.wait_recv()
            for h in range(heads):
                if i:
                    before = state(chain_c, chain_aux, h)
                else:
                    other = state(other_c, other_aux, h)
                    before = [jnp.zeros_like(a) for a in other]
                after_other = joined(before, state(other_c, other_aux, h))
                put(in_c, in_aux, h, [jnp.where(side == 0, a, b) for a, b in zip(before, after_other)])
                if i + 1 < half:
                    put(next_c, next_aux, h, joined(before, state(pair_c, pair_aux, h)))
            if i + 1 < half:
                for copy in chain_copies:
                    copy.start()

    in_aux[...] = jnp.zeros_like(in_aux)
    next_aux[...] = jnp.zeros_like(next_aux)
    pair_aux[...] = jnp.zeros_like(pair_aux)
    for copy in pair_copies:
        copy.start()
    for k in range(half):
        out_copy(k + half).start()
        if k:
            out_copy(k).start()
    for copy in weights:
        copy.start()

    def spread_own(i):
        for k in (i, i + half):
            if k:
                out_copy(k).wait_recv()
            else:
                local.wait()
            to_across(k).start()
            to_partner_own(k).start()

    def spread_far(i):
        for k in (i, i + half):
            to_across(k).wait_recv()
            to_partner_far(k).start()

    def all_here(i):
        for k in (i, i + half):
            to_partner_own(k).wait_recv()
            to_partner_far(k).wait_recv()

    def wide(block):
        return block.astype(jnp.float32)

    def sum_pairs(i):
        for k in (i, i + half):
            sum_to_partner(k).wait_recv()
            pair_sum[k] = (wide(part[k, 1]) + wide(first[k, 1])).astype(jnp.bfloat16)
            sum_across(k).start()

    def sum_rest(i):
        for k in (i, i + half):
            sum_across(k).wait_recv()
            done = (wide(part[k, 0]) + wide(first[k, 0]) + wide(second[k])).astype(jnp.bfloat16)
            if k:
                final[k] = done
                give_back(k).start()
            else:
                ret_ref[0] = done

    def hidden_units(i):
        for at, k in enumerate((i, i + half)):
            block = jnp.concatenate([wide(disp[k, j]) for j in range(4)], axis=0)
            rows_in[pl.ds(at * 4 * cap, 4 * cap)] = block.astype(jnp.bfloat16)

        def step(j, carry):
            both = jnp.dot(rows_in[...], gate_up[j], preferred_element_type=jnp.float32)
            gate_out, up_out = both[:, :LANES], both[:, LANES:]
            hidden[j] = (jax.nn.silu(gate_out) * up_out).astype(jnp.bfloat16)
            return carry

        lax.fori_loop(0, tiles, step, 0)

    def results(i):
        units = jnp.concatenate([hidden[j] for j in range(tiles)], axis=1)

        def step(j, carry):
            out = jnp.dot(units, down[j], preferred_element_type=jnp.float32)
            cols = pl.ds(pl.multiple_of(j * out_cols, out_cols), out_cols)
            for at, k in enumerate((i, i + half)):
                for m in range(4):
                    lo = (at * 4 + m) * cap
                    part[k, m, :, cols] = out[lo : lo + cap].astype(jnp.bfloat16)
            return carry

        lax.fori_loop(0, outs, step, 0)

    spread_own(0)
    spread_far(0)
    for i in range(half):
        all_here(i)
        if i == 0:
            for copy in weights:
                copy.wait()
        if i + 1 < half:
            spread_own(i + 1)
        hidden_units(i)
        if i:
            sum_pairs(i - 1)
        results(i)
        for k in (i, i + half):
            sum_to_partner(k).start()
        if i == 0:
            pair_total()
        chain(i)
        if i + 1 < half:
            spread_far(i + 1)
        if i:
            sum_rest(i - 1)
    sum_pairs(half - 1)
    sum_rest(half - 1)
    for copy in pair_copies:
        copy.wait_send()

    @pl.when(step_at < half - 1)
    def _():
        for copy in chain_copies:
            copy.wait_send()

    for k in range(n_ep):
        if k:
            give_back(k).wait_recv()
            out_copy(k).wait_send()
            give_back(k).wait_send()
        to_across(k).wait_send()
        to_partner_own(k).wait_send()
        to_partner_far(k).wait_send()
        sum_to_partner(k).wait_send()
        sum_across(k).wait_send()


def experts_by_kernel(sendbuf, state, gate_matrix, up_matrix, down_matrix, n_ep):
    cell, norm, stab, total = state
    heads, size = norm.shape
    spread = lambda part: jnp.broadcast_to(part[:, None], (heads, size))
    aux = jnp.concatenate([norm, spread(stab), spread(total)], axis=0)
    aux = jnp.pad(aux, ((0, -aux.shape[0] % 8), (0, 0)))
    rows, width = sendbuf.shape
    cap = rows // n_ep
    units = gate_matrix.shape[1]
    tiles, out_cols = units // LANES, 256
    block = (n_ep, cap, width)
    vmem = pltpu.VMEM
    bf16 = jnp.bfloat16
    dma = pltpu.SemaphoreType.DMA
    c_shape = (heads * size, size)
    returned, in_c, in_aux = pl.pallas_call(
        functools.partial(expert_kernel, n_ep, heads),
        out_shape=(
            jax.ShapeDtypeStruct(block, bf16),
            jax.ShapeDtypeStruct(c_shape, jnp.float32),
            jax.ShapeDtypeStruct(aux.shape, jnp.float32),
        ),
        in_specs=[pl.BlockSpec(memory_space=pltpu.VMEM)] * 3 + [pl.BlockSpec(memory_space=pl.ANY)] * 3,
        out_specs=[pl.BlockSpec(memory_space=pltpu.VMEM)] * 3,
        scratch_shapes=[
            vmem((n_ep, 4, cap, width), bf16),
            vmem((n_ep, 4, cap, width), bf16),
            vmem((n_ep, 2, cap, width), bf16),
            vmem(block, bf16),
            vmem(block, bf16),
            vmem(block, bf16),
            vmem((8 * cap, width), bf16),
            vmem((tiles, 8 * cap, LANES), bf16),
            vmem((tiles, width, 2 * LANES), bf16),
            vmem((width // out_cols, units, out_cols), bf16),
            vmem(c_shape, bf16),
            vmem(aux.shape, jnp.float32),
            vmem(c_shape, jnp.float32),
            vmem(aux.shape, jnp.float32),
            vmem(c_shape, bf16),
            vmem(aux.shape, jnp.float32),
            vmem(c_shape, bf16),
            vmem(aux.shape, jnp.float32),
            dma((4,)),
            dma((4,)),
            dma((3 * tiles + width // out_cols,)),
            dma,
        ]
        + [dma((n_ep,))] * 14,
        compiler_params=pltpu.CompilerParams(
            collective_id=0, has_side_effects=True, vmem_limit_bytes=56 * 1024 * 1024
        ),
        cost_estimate=pl.CostEstimate(
            flops=24 * rows * width * units, bytes_accessed=6 * width * units, transcendentals=4 * rows * units
        ),
    )(
        sendbuf.reshape(block),
        cell.astype(bf16).reshape(c_shape),
        aux,
        gate_matrix,
        up_matrix,
        down_matrix,
    )
    prior = (
        in_c.reshape(heads, size, size),
        in_aux[:heads],
        in_aux[heads : 2 * heads, 0],
        in_aux[2 * heads : 3 * heads, 0],
    )
    return returned.reshape(rows, width), prior


def local(
    cell_query_rows,
    cell_key_rows,
    cell_value_rows,
    output_gate_logits,
    log_input_gate,
    forget_gate_logits,
    extra_log_forget,
    cell_output_scale,
    tokens_into_experts,
    expert_norm_scale,
    token_expert_index,
    chosen_expert_weight,
    expert_gate_weight,
    expert_up_weight,
    expert_down_weight,
):
    ep_count = lax.axis_size("ep")
    n_tok = tokens_into_experts.shape[0]
    experts = ep_count * expert_gate_weight.shape[0]
    capacity = n_tok * TOPK * 5 // (4 * experts)
    input_float = tokens_into_experts.astype(jnp.float32)
    normed = (
        input_float
        * lax.rsqrt(jnp.mean(input_float * input_float, axis=-1, keepdims=True) + EPSILON)
        * expert_norm_scale
    ).astype(jnp.bfloat16)
    gate_matrix = expert_gate_weight[0]
    up_matrix = expert_up_weight[0]
    down_matrix = expert_down_weight[0]
    by_kernel = (
        lax.axis_size("tp") == 4
        and ep_count % 2 == 0
        and capacity % 8 == 0
        and gate_matrix.shape[1] % LANES == 0
        and gate_matrix.shape[0] % 256 == 0
    )
    if by_kernel:
        token_expert_index = (token_expert_index + ep_count - lax.axis_index("ep")) % ep_count
    hit, chosen = slot_masks(token_expert_index, experts, capacity)
    sendbuf = lax.dot_general(
        hit.astype(jnp.bfloat16), normed, (((0,), (0,)), ((), ())), preferred_element_type=jnp.float32
    ).astype(jnp.bfloat16)
    if by_kernel:
        box = []

        def carry(device_total):
            returned, prior = experts_by_kernel(
                sendbuf, device_total, gate_matrix, up_matrix, down_matrix, ep_count
            )
            box.append(returned)
            return prior

    else:
        carry = gathered_carry
    gated_head_output = mix_heads(
        cell_query_rows,
        cell_key_rows,
        cell_value_rows,
        output_gate_logits,
        log_input_gate,
        forget_gate_logits,
        extra_log_forget,
        cell_output_scale,
        carry,
    )
    if by_kernel:
        (returned,) = box
    else:
        arrived = lax.all_to_all(sendbuf, "ep", split_axis=0, concat_axis=0, tiled=True)
        routed_rows = lax.all_gather(arrived, "tp", axis=0, tiled=True)
        gate_out = jnp.dot(routed_rows, gate_matrix, preferred_element_type=jnp.float32)
        up_out = jnp.dot(routed_rows, up_matrix, preferred_element_type=jnp.float32)
        hidden = (jax.nn.silu(gate_out) * up_out).astype(jnp.bfloat16)
        summed = lax.psum_scatter(
            jnp.dot(hidden, down_matrix, preferred_element_type=jnp.float32).astype(jnp.bfloat16),
            "tp",
            scatter_dimension=0,
            tiled=True,
        )
        returned = lax.all_to_all(summed, "ep", split_axis=0, concat_axis=0, tiled=True)
    slot_weight = sum(
        jnp.where(jnp.logical_and(hit, named), chosen_expert_weight[:, j : j + 1], 0.0)
        for j, named in enumerate(chosen)
    )
    expert_output = jnp.dot(
        slot_weight,
        returned.astype(jnp.float32),
        precision=lax.Precision.HIGHEST,
        preferred_element_type=jnp.float32,
    ).astype(jnp.bfloat16)
    return (gated_head_output, expert_output)


def solution(mesh):
    return jax.shard_map(
        local,
        mesh=mesh,
        in_specs=(
            P("ep", "tp"),
            P("ep", "tp"),
            P("ep", "tp"),
            P("ep", "tp"),
            P("tp", "ep"),
            P("tp", "ep"),
            P("tp", "ep"),
            P("tp"),
            P(("ep", "tp"), None),
            P(),
            P(("ep", "tp"), None),
            P(("ep", "tp"), None),
            P("ep", None, "tp"),
            P("ep", None, "tp"),
            P("ep", "tp", None),
        ),
        out_specs=(P("ep", "tp"), P(("ep", "tp"), None)),
        check_vma=False,
    )
```
